32 devices in a mesh: ep: 32 (over z, y, x, core).
Axes of the slice: x: 2, y: 2, z: 4, core: 2. Of those that a mesh axis runs over, the one named last changes fastest.
Arguments:
- tokens: bfloat16 [256, 2048], P('ep'), may hold values from -6 to 6
- norm_gain: float32 [2048], replicated, may hold values from 0.1 to 1.9
- expert_gate: bfloat16 [32, 2048, 640], P('ep'), may hold values from -0.125 to 0.125
- expert_up: bfloat16 [32, 2048, 640], P('ep'), may hold values from -0.125 to 0.125
- expert_down: bfloat16 [32, 640, 2048], P('ep'), may hold values from -0.25 to 0.25
- shared_gate: bfloat16 [2048, 512], P(None, 'ep'), may hold values from -0.125 to 0.125
- shared_up: bfloat16 [2048, 512], P(None, 'ep'), may hold values from -0.125 to 0.125
- shared_down: bfloat16 [512, 2048], P('ep'), may hold values from -0.25 to 0.25
- branch_gate: bfloat16 [2048], replicated, may hold values from -0.125 to 0.125
- route_expert: int32 [256, 8], P('ep'), may hold values from 0 to 31, all different within a row; in each aligned block of 8 rows (0 to 7, 8 to 15, ...) at most 2 rows name the same one
- route_weight: float32 [256, 8], P('ep'), may hold values from 0.05 to 0.5
Outputs:
- mixed: bfloat16 [256, 2048], P('ep')
The draws below stay inside these ranges and needn't reach their ends.
Inputs may be any that keep to these rules, and one draw needn't show every extreme that they name: `route_expert`: each row names 8 different experts; the rows of one device name one expert at most 2 times.
All inputs are finite; a program needn't handle non-finite values.
Results may differ from the reference program's by a relative error of at most 0.0085.
Values may be sent and summed in bfloat16 or wider, within the bound.
A program may use at most 128 MiB of HBM per device.

```python
import math
import jax
import jax.numpy as jnp
import numpy as np
from jax import lax

D = 2048
FF_E = 640
TOPK = 8
TOK_DEV = 8
EXPERTS = 32
SHARED = 512
TOKENS = 256
CAP = 2
N_EP = 32


def level_of(key, shape, shards, low, high):
    gain = 1.0
    for position, parts in shards:
        draws = jax.random.uniform(jax.random.fold_in(jax.random.fold_in(key, 6), position), (parts,), jnp.float32, low / len(shards), high / len(shards))
        gain = gain * jnp.repeat(jnp.exp(draws), shape[position] // parts).reshape((-1,) + (1,) * (len(shape) - 1 - position))
    return gain


def assign_block(rng, own, number, rows, count, top, most, lean):
    ranking = jax.random.permutation(rng, count)
    heavy_load, usual = portions_of(count, rows * top, most, lean, True), portions_of(count, rows * top, most, lean, False)
    places = jnp.arange(count)

    def named(sizes, offset_by):
        used = int((sizes > 0).sum())
        fixed = max(1, used // 4)
        shifted = fixed + (places - fixed + offset_by * (used - fixed)) % max(1, count - fixed)
        return jnp.zeros((count,), jnp.int32).at[ranking[jnp.where(places < fixed, places, shifted)]].set(jnp.asarray(sizes, jnp.int32))

    sizes = jnp.where(number % 4 == 0, named(heavy_load, number // 4), named(usual, number - number // 4 - 1))
    mixed = jax.random.permutation(jax.random.fold_in(own, 3), count)
    giver, taker = mixed[0:count // 2 * 2:2], mixed[1:count // 2 * 2:2]
    slack = jnp.minimum(sizes[giver] - 1, most - sizes[taker]) // 2
    slack = jnp.where((giver == ranking[0]) | (taker == ranking[0]) | (sizes[taker] == 0), 0, jnp.maximum(slack, 0))
    shifted = jax.random.randint(jax.random.fold_in(own, 4), (count // 2,), 0, 1 << 20) % (slack + 1)
    sizes = sizes.at[giver].add(-shifted).at[taker].add(shifted)
    members = jnp.searchsorted(jnp.cumsum(sizes), jnp.arange(rows * top), side="right").astype(jnp.int32)
    table = members.reshape(top, rows).T
    table = table[jax.random.permutation(jax.random.fold_in(own, 1), rows)]
    offset_by = jax.random.randint(jax.random.fold_in(own, 2), (rows, 1), 0, top)
    return jnp.take_along_axis(table, (jnp.arange(top)[None, :] + offset_by) % top, axis=1)


def portions_of(count, total, reach, skew, full):
    loads = [(1 << 20) // math.isqrt(standing ** skew) + 1 for standing in range(1, count + 1)]
    largest = reach if full else min(reach, max(-(-total // count), total * loads[0] // sum(loads)))
    least = 1 if total - largest >= count - 1 else 0
    given, rest = [largest] + [least] * (count - 1), total - largest - least * (count - 1)
    while rest > 0:
        free = [i for i in range(1, count) if given[i] < largest] or [i for i in range(1, count) if given[i] < reach]
        whole, budget = sum([loads[i] for i in free]), rest
        for i in free:
            addition = min(reach - given[i], max(1, budget * loads[i] // whole), rest)
            given[i] = given[i] + addition
            rest = rest - addition
    return np.array(given)


def gaussian(rng, dims, deviation, bound, pieces=(), held_as=jnp.bfloat16):
    result = deviation * jax.random.normal(rng, dims, jnp.float32)
    if pieces:
        result = result * level_of(rng, dims, pieces, -0.22, 0.18)
    return jnp.clip(result, -bound, bound).astype(held_as)


def setup_inputs(seed: int = 0) -> dict:
    key_list = jax.random.split(jax.random.key(seed), 12)
    tokens = gaussian(key_list[0], (TOKENS, D), 1.0, 6.0, ((0, 32),))
    norm_gain = jnp.clip(1.0 + 0.18 * jax.random.normal(key_list[1], (D,), jnp.float32), 0.1, 1.9)
    expert_gate = gaussian(key_list[2], (EXPERTS, D, FF_E), D ** -0.5, 0.125, ((0, 32),))
    expert_up = gaussian(key_list[3], (EXPERTS, D, FF_E), D ** -0.5, 0.125, ((0, 32),))
    expert_down = gaussian(key_list[4], (EXPERTS, FF_E, D), FF_E ** -0.5, 0.25, ((0, 32),))
    shared_gate = gaussian(key_list[5], (D, SHARED), D ** -0.5, 0.125, ((1, 32),))
    shared_up = gaussian(key_list[6], (D, SHARED), D ** -0.5, 0.125, ((1, 32),))
    shared_down = gaussian(key_list[7], (SHARED, D), SHARED ** -0.5, 0.25, ((0, 32),))
    branch_gate = gaussian(key_list[8], (D,), D ** -0.5, 0.125)
    route_expert_keys = jax.random.split(jax.random.fold_in(key_list[9], 1), TOKENS // TOK_DEV)
    route_expert_turns = jax.random.permutation(jax.random.fold_in(key_list[9], 3), TOKENS // TOK_DEV)
    route_expert = jax.vmap(lambda own, number: assign_block(jax.random.fold_in(key_list[9], 2), own, number, TOK_DEV, EXPERTS, TOPK, CAP, 2))(route_expert_keys, route_expert_turns).reshape((TOKENS, TOPK))
    route_weight = jnp.clip(0.05 + 0.45 * jax.random.uniform(key_list[10], (TOKENS, TOPK), jnp.float32) ** level_of(key_list[10], (TOKENS, TOPK), ((0, 32),), -0.2, 0.2), 0.05, 0.5)
    return dict(tokens=tokens, norm_gain=norm_gain, expert_gate=expert_gate, expert_up=expert_up, expert_down=expert_down, shared_gate=shared_gate, shared_up=shared_up, shared_down=shared_down, branch_gate=branch_gate, route_expert=route_expert, route_weight=route_weight)


def norm_rows(tokens, norm_gain):
    values = tokens.astype(jnp.float32)
    scale = lax.rsqrt(lax.optimization_barrier(jnp.mean(values * values, axis=-1, keepdims=True)) + 1e-06)
    return (values * scale * norm_gain).astype(jnp.bfloat16)

def reference(tokens, norm_gain, expert_gate, expert_up, expert_down, shared_gate, shared_up, shared_down, branch_gate, route_expert, route_weight):
    normed = norm_rows(tokens, norm_gain)
    limit = N_EP * CAP
    count = normed.shape[0]
    positions = jnp.arange(count, dtype=jnp.int32)

    def one_expert(total, inputs):
        number, w_gate, w_up, w_down = inputs
        match = route_expert == number
        hit = jnp.any(match, axis=1)
        weight = lax.optimization_barrier(jnp.sum(jnp.where(match, route_weight, jnp.float32(0.0)), axis=1))
        order = jnp.cumsum(hit.astype(jnp.int32)) - 1
        target = jnp.where(hit, order, limit).astype(jnp.int32)
        index = jnp.zeros((limit,), jnp.int32).at[target].set(positions, mode='drop')
        slot_weight = jnp.zeros((limit,), jnp.float32).at[target].set(weight, mode='drop')
        rows = normed[index]
        hidden = (jax.nn.silu(jnp.dot(rows, w_gate, preferred_element_type=jnp.float32)) * jnp.dot(rows, w_up, preferred_element_type=jnp.float32)).astype(jnp.bfloat16)
        output = jnp.dot(hidden, w_down, preferred_element_type=jnp.float32).astype(jnp.bfloat16)
        total = total.at[index].add(slot_weight[:, None] * output.astype(jnp.float32))
        return (total, None)
    numbers = jnp.arange(expert_gate.shape[0], dtype=jnp.int32)
    start = jnp.zeros((count, normed.shape[1]), jnp.float32)
    moe, unused = lax.scan(one_expert, start, (numbers, expert_gate, expert_up, expert_down))
    dense_hidden = (jax.nn.silu(jnp.dot(normed, shared_gate, preferred_element_type=jnp.float32)) * jnp.dot(normed, shared_up, preferred_element_type=jnp.float32)).astype(jnp.bfloat16)
    dense = jnp.dot(dense_hidden, shared_down, preferred_element_type=jnp.float32)
    gate = jax.nn.sigmoid(jnp.dot(normed, branch_gate, preferred_element_type=jnp.float32))
    return (moe + gate[:, None] * dense).astype(jnp.bfloat16)
```

```python
import functools

import jax
import jax.numpy as jnp
from jax import lax
from jax.experimental import pallas as pl
from jax.experimental.pallas import tpu as pltpu
from jax.sharding import PartitionSpec as P

F32 = jnp.float32
BF16 = jnp.bfloat16


def silu_pair(gate, up):
    return (gate / (1.0 + jnp.exp(-gate)) * up).astype(BF16)


def kernel(
    n,
    tokens,
    gain,
    branch,
    route,
    weight,
    e_gate,
    e_up,
    e_down,
    s_gate,
    s_up,
    s_down,
    out,
    toks,
    side,
    wg,
    wu,
    wd,
    sgu,
    sd,
    mine,
    theirs,
    given,
    sending,
    landed,
    w_sem,
    ts,
    tr,
    ss,
    sr,
    fts,
    ftr,
    fss,
    fsr,
    ps,
    pr,
    rs,
    rr,
):
    half = n // 2
    me = lax.axis_index("ep")
    core = lax.rem(me, 2)
    chip = me // 2
    partner = me + 1 - 2 * core

    loads = [
        pltpu.make_async_copy(src, dst, w_sem.at[i])
        for i, (src, dst) in enumerate(
            (
                (e_gate.at[0], wg),
                (e_up.at[0], wu),
                (s_gate, sgu.at[0]),
                (s_up, sgu.at[1]),
                (s_down, sd),
                (e_down.at[0], wd),
            )
        )
    ]
    for load in loads:
        load.start()

    def device_at(d):
        return lax.rem(chip + d, half) * 2 + core

    barrier = pltpu.get_barrier_semaphore()

    @pl.loop(1, half)
    def _(d):
        pl.semaphore_signal(barrier, inc=1, device_id={"ep": device_at(d)})

    pl.semaphore_signal(barrier, inc=1, device_id={"ep": partner})

    values = tokens[...].astype(F32)
    scale = lax.rsqrt(jnp.mean(values * values, axis=-1, keepdims=True) + 1e-06)
    normed = (values * scale * gain[...]).astype(BF16)
    toks[0, 0] = normed
    score = jnp.sum(normed.astype(F32) * branch[...].astype(F32).reshape(1, -1), axis=-1, keepdims=True)
    lane = lax.broadcasted_iota(jnp.int32, side.shape[2:], 1)
    table = jnp.where(lane == n, 1.0 / (1.0 + jnp.exp(-score)), 0.0)
    for k in range(route.shape[1]):
        table += jnp.where(lane == route[:, k : k + 1], weight[:, k : k + 1], 0.0)
    side[0, 0] = table

    pl.semaphore_wait(barrier, half)

    def spread(d):
        to = {"ep": device_at(d)}
        return (
            pltpu.make_async_remote_copy(
                toks.at[0, 0], toks.at[0, d], ts.at[d], tr.at[d], device_id=to
            ),
            pltpu.make_async_remote_copy(
                side.at[0, 0], side.at[0, d], ss.at[d], sr.at[d], device_id=to
            ),
        )

    def forward(d):
        to = {"ep": partner}
        return (
            pltpu.make_async_remote_copy(
                toks.at[0, d], toks.at[1, d], fts.at[d], ftr.at[d], device_id=to
            ),
            pltpu.make_async_remote_copy(
                side.at[0, d], side.at[1, d], fss.at[d], fsr.at[d], device_id=to
            ),
        )

    @pl.loop(1, half)
    def _(d):
        for copy in spread(d):
            copy.start()

    for copy in forward(0):
        copy.start()

    @pl.loop(1, half)
    def _(d):
        for copy in spread(d):
            copy.wait_recv()
        for copy in forward(d):
            copy.start()

    for load in loads:
        load.wait()

    @pl.loop(0, half)
    def _(d):
        for copy in forward(d):
            copy.wait_recv()

    def combined(which):
        rows = half * toks.shape[2]
        x = toks[which].reshape(rows, toks.shape[3])
        facts = side[which].reshape(rows, side.shape[3])
        spot = lax.broadcasted_iota(jnp.int32, facts.shape, 1)
        share = jnp.sum(jnp.where(spot == me, facts, 0.0), axis=1, keepdims=True)
        gate = jnp.sum(jnp.where(spot == n, facts, 0.0), axis=1, keepdims=True)
        dot = functools.partial(jnp.dot, preferred_element_type=F32)
        hidden = silu_pair(dot(x, wg[...]), dot(x, wu[...]))
        units = sgu.shape[1]
        pair = lax.dot_general(
            x,
            sgu[...].reshape(2 * units, sgu.shape[2]),
            (((1,), (1,)), ((), ())),
            preferred_element_type=F32,
        )
        dense_hidden = silu_pair(pair[:, :units], pair[:, units:])
        routed = dot(hidden, wd[...]).astype(BF16).astype(F32)
        return share * routed + gate * dot(dense_hidden, sd[...])

    theirs[...] = combined(1).astype(BF16).reshape(theirs.shape)
    swap = pltpu.make_async_remote_copy(
        theirs, given, ps, pr, device_id={"ep": partner}
    )
    swap.start()
    mine[...] = combined(0).reshape(mine.shape)
    swap.wait_recv()
    total = mine[...] + given[...].astype(F32)
    sending[...] = total.astype(BF16)

    def home(d):
        return pltpu.make_async_remote_copy(
            sending.at[d],
            landed.at[d],
            rs.at[d],
            rr.at[d],
            device_id={"ep": lax.rem(chip - d + half, half) * 2 + core},
        )

    @pl.loop(1, half)
    def _(d):
        home(d).start()

    mine[0] = total[0]

    @pl.loop(1, half)
    def _(d):
        for copy in spread(d):
            copy.wait_send()

    @pl.loop(0, half)
    def _(d):
        for copy in forward(d):
            copy.wait_send()

    swap.wait_send()

    @pl.loop(1, half)
    def _(d):
        home(d).wait_recv()
        mine[0] += landed[d].astype(F32)

    out[...] = mine[0].astype(BF16)

    @pl.loop(1, half)
    def _(d):
        home(d).wait_send()


def per_device(
    tokens,
    norm_gain,
    expert_gate,
    expert_up,
    expert_down,
    shared_gate,
    shared_up,
    shared_down,
    branch_gate,
    route_expert,
    route_weight,
):
    n = lax.axis_size("ep")
    half = n // 2
    rows, width = tokens.shape
    lanes = (n + 1 + 127) // 128 * 128
    vmem = pl.BlockSpec(memory_space=pltpu.VMEM)
    anywhere = pl.BlockSpec(memory_space=pl.ANY)
    dma = pltpu.SemaphoreType.DMA
    return pl.pallas_call(
        functools.partial(kernel, n),
        out_shape=jax.ShapeDtypeStruct((rows, width), BF16),
        in_specs=[vmem] * 5 + [anywhere] * 6,
        out_specs=vmem,
        scratch_shapes=[
            pltpu.VMEM((2, half, rows, width), BF16),
            pltpu.VMEM((2, half, rows, lanes), F32),
            pltpu.VMEM(expert_gate.shape[1:], BF16),
            pltpu.VMEM(expert_up.shape[1:], BF16),
            pltpu.VMEM(expert_down.shape[1:], BF16),
            pltpu.VMEM((2,) + shared_gate.shape[::-1], BF16),
            pltpu.VMEM(shared_down.shape, BF16),
            pltpu.VMEM((half, rows, width), F32),
            pltpu.VMEM((half, rows, width), BF16),
            pltpu.VMEM((half, rows, width), BF16),
            pltpu.VMEM((half, rows, width), BF16),
            pltpu.VMEM((half, rows, width), BF16),
            dma((6,)),
        ]
        + [dma((half,))] * 8
        + [dma, dma]
        + [dma((half,))] * 2,
        compiler_params=pltpu.CompilerParams(
            collective_id=0, has_side_effects=True, vmem_limit_bytes=60 * 1024 * 1024
        ),
    )(
        tokens,
        norm_gain.reshape(1, -1),
        branch_gate,
        route_expert,
        route_weight,
        expert_gate,
        expert_up,
        expert_down,
        shared_gate.T,
        shared_up.T,
        shared_down,
    )


def solution(mesh):
    placed = (
        P("ep", None),
        P(),
        P("ep", None, None),
        P("ep", None, None),
        P("ep", None, None),
        P(None, "ep"),
        P(None, "ep"),
        P("ep", None),
        P(),
        P("ep", None),
        P("ep", None),
    )
    return jax.shard_map(
        per_device, mesh=mesh, in_specs=placed, out_specs=P("ep", None), check_vma=False
    )
```

```python
import functools
import math

import jax
import jax.numpy as jnp
from jax import lax
from jax.experimental import pallas as pl
from jax.experimental.pallas import tpu as pltpu
from jax.sharding import PartitionSpec as P

F32 = jnp.float32
BF16 = jnp.bfloat16


def silu_pair(gate, up):
    return (gate / (1.0 + jnp.exp(-gate)) * up).astype(BF16)


def kernel(
    n,
    plane,
    tokens,
    gain,
    branch,
    route,
    weight,
    e_gate,
    e_up,
    e_down,
    s_gate,
    s_up,
    s_down,
    out,
    toks,
    wg,
    wu,
    wd,
    sgu,
    sd,
    mine,
    theirs,
    given,
    sending,
    landed,
    summed,
    arrived,
    w_sem,
    far_s,
    far_r,
    near_s,
    near_r,
    pass_s,
    pass_r,
    swap_s,
    swap_r,
    part_s,
    part_r,
    last_s,
    last_r,
):
    half = n // 2
    planes = half // plane
    width = tokens.shape[1]
    me = lax.axis_index("ep")
    core = lax.rem(me, 2)
    chip = me // 2
    low = lax.rem(chip, plane)
    high = chip // plane
    partner = {"ep": me + 1 - 2 * core}

    def at(a, b):
        row = lax.rem(high + a + planes, planes)
        column = lax.rem(low + b + plane, plane)
        return {"ep": (row * plane + column) * 2 + core}

    loads = [
        pltpu.make_async_copy(src, dst, w_sem.at[i])
        for i, (src, dst) in enumerate(
            (
                (e_gate.at[0], wg),
                (e_up.at[0], wu),
                (s_gate, sgu.at[0]),
                (s_up, sgu.at[1]),
                (s_down, sd),
                (e_down.at[0], wd),
            )
        )
    ]
    for load in loads:
        load.start()

    barrier = pltpu.get_barrier_semaphore()
    for a in range(1, planes):
        pl.semaphore_signal(barrier, inc=1, device_id=at(a, 0))
    for b in range(1, plane):
        pl.semaphore_signal(barrier, inc=1, device_id=at(0, b))
    pl.semaphore_signal(barrier, inc=1, device_id=partner)

    values = tokens[...].astype(F32)
    scale = lax.rsqrt(jnp.mean(values * values, axis=-1, keepdims=True) + 1e-06)
    normed = (values * scale * gain[...]).astype(BF16)
    score = jnp.sum(
        normed.astype(F32) * branch[...].astype(F32).reshape(1, -1), axis=-1, keepdims=True
    )

    def columns(shape):
        lane = lax.broadcasted_iota(jnp.int32, shape, 1)
        piece = (lane >= n + 1).astype(jnp.int32) + (lane >= 2 * (n + 1)).astype(jnp.int32)
        return piece, lane - piece * (n + 1)

    piece, column = columns((tokens.shape[0], toks.shape[4] - width))
    table = jnp.where(column == n, 1.0 / (1.0 + jnp.exp(-score)), 0.0)
    for k in range(route.shape[1]):
        table += jnp.where(column == route[:, k : k + 1], weight[:, k : k + 1], 0.0)
    first = table.astype(BF16).astype(F32)
    second = (table - first).astype(BF16).astype(F32)
    third = table - first - second
    pieces = jnp.where(piece == 0, first, jnp.where(piece == 1, second, third))
    toks[0, 0, 0, :, :width] = normed
    toks[0, 0, 0, :, width:] = pieces.astype(BF16)

    pl.semaphore_wait(barrier, planes + plane - 1)

    def far(a):
        return pltpu.make_async_remote_copy(
            toks.at[0, 0, 0],
            toks.at[0, 0, a],
            far_s.at[a],
            far_r.at[a],
            device_id=at(-a, 0),
        )

    def near(a, b):
        return pltpu.make_async_remote_copy(
            toks.at[0, 0, a],
            toks.at[0, b, a],
            near_s.at[b, a],
            near_r.at[b, a],
            device_id=at(0, -b),
        )

    def hand(a, b):
        return pltpu.make_async_remote_copy(
            toks.at[0, b, a],
            toks.at[1, b, a],
            pass_s.at[b, a],
            pass_r.at[b, a],
            device_id=partner,
        )

    order = sorted(range(1, planes), key=lambda a: min(a, planes - a))
    for a in order:
        far(a).start()
    for b in range(1, plane):
        near(0, b).start()
    hand(0, 0).start()
    for a in order:
        far(a).wait_recv()
        for b in range(1, plane):
            near(a, b).start()
        hand(a, 0).start()
    for a in [0] + order:
        for b in range(1, plane):
            near(a, b).wait_recv()
            hand(a, b).start()

    for load in loads:
        load.wait()

    for a in range(planes):
        for b in range(plane):
            hand(a, b).wait_recv()

    def combined(which):
        rows = half * tokens.shape[0]
        x = toks[which, :, :, :, :width].reshape(rows, width)
        facts = toks[which, :, :, :, width:].astype(F32).reshape(rows, -1)
        _, spot = columns(facts.shape)
        share = jnp.sum(jnp.where(spot == me, facts, 0.0), axis=1, keepdims=True)
        gate = jnp.sum(jnp.where(spot == n, facts, 0.0), axis=1, keepdims=True)
        dot = functools.partial(jnp.dot, preferred_element_type=F32)
        hidden = silu_pair(dot(x, wg[...]), dot(x, wu[...]))
        units = sgu.shape[1]
        pair = lax.dot_general(
            x,
            sgu[...].reshape(2 * units, width),
            (((1,), (1,)), ((), ())),
            preferred_element_type=F32,
        )
        dense_hidden = silu_pair(pair[:, :units], pair[:, units:])
        routed = dot(hidden, wd[...]).astype(BF16).astype(F32)
        return share * routed + gate * dot(dense_hidden, sd[...])

    theirs[...] = combined(1).astype(BF16).reshape(theirs.shape)
    swap = pltpu.make_async_remote_copy(theirs, given, swap_s, swap_r, device_id=partner)
    swap.start()
    mine[...] = combined(0).reshape(mine.shape)
    swap.wait_recv()
    for b in range(1, plane):
        sending[b] = (mine[b] + given[b].astype(F32)).astype(BF16)

    def part(a, b):
        return pltpu.make_async_remote_copy(
            sending.at[b, a],
            landed.at[b, a],
            part_s.at[b, a],
            part_r.at[b, a],
            device_id=at(0, b),
        )

    def last(a):
        return pltpu.make_async_remote_copy(
            summed.at[a], arrived.at[a], last_s.at[a], last_r.at[a], device_id=at(a, 0)
        )

    back = order[::-1]
    for a in back + [0]:
        for b in range(1, plane):
            part(a, b).start()

    def whole(a):
        total = mine[0, a] + given[0, a].astype(F32)
        for b in range(1, plane):
            part(a, b).wait_recv()
            total += landed[b, a].astype(F32)
        return total

    for a in back:
        summed[a] = whole(a).astype(BF16)
        last(a).start()
    result = whole(0)

    for a in order:
        far(a).wait_send()
    for a in range(planes):
        for b in range(plane):
            hand(a, b).wait_send()
            if b > 0:
                near(a, b).wait_send()
                part(a, b).wait_send()
    swap.wait_send()

    for a in back:
        last(a).wait_recv()
        result += arrived[a].astype(F32)
    out[...] = result.astype(BF16)
    for a in back:
        last(a).wait_send()


def per_device(
    tokens,
    norm_gain,
    expert_gate,
    expert_up,
    expert_down,
    shared_gate,
    shared_up,
    shared_down,
    branch_gate,
    route_expert,
    route_weight,
):
    n = lax.axis_size("ep")
    half = n // 2
    plane = math.isqrt(half)
    while half % plane:
        plane -= 1
    planes = half // plane
    rows, width = tokens.shape
    lanes = (3 * (n + 1) + 127) // 128 * 128
    vmem = pl.BlockSpec(memory_space=pltpu.VMEM)
    anywhere = pl.BlockSpec(memory_space=pl.ANY)
    dma = pltpu.SemaphoreType.DMA
    blocks = pltpu.VMEM((plane, planes, rows, width), BF16)
    return pl.pallas_call(
        functools.partial(kernel, n, plane),
        out_shape=jax.ShapeDtypeStruct((rows, width), BF16),
        in_specs=[vmem] * 5 + [anywhere] * 6,
        out_specs=vmem,
        scratch_shapes=[
            pltpu.VMEM((2, plane, planes, rows, width + lanes), BF16),
            pltpu.VMEM(expert_gate.shape[1:], BF16),
            pltpu.VMEM(expert_up.shape[1:], BF16),
            pltpu.VMEM(expert_down.shape[1:], BF16),
            pltpu.VMEM((2,) + shared_gate.shape[::-1], BF16),
            pltpu.VMEM(shared_down.shape, BF16),
            pltpu.VMEM((plane, planes, rows, width), F32),
            blocks,
            blocks,
            blocks,
            blocks,
            pltpu.VMEM((planes, rows, width), BF16),
            pltpu.VMEM((planes, rows, width), BF16),
            dma((6,)),
            dma((planes,)),
            dma((planes,)),
            dma((plane, planes)),
            dma((plane, planes)),
            dma((plane, planes)),
            dma((plane, planes)),
            dma,
            dma,
            dma((plane, planes)),
            dma((plane, planes)),
            dma((planes,)),
            dma((planes,)),
        ],
        compiler_params=pltpu.CompilerParams(
            collective_id=0, has_side_effects=True, vmem_limit_bytes=60 * 1024 * 1024
        ),
    )(
        tokens,
        norm_gain.reshape(1, -1),
        branch_gate,
        route_expert,
        route_weight,
        expert_gate,
        expert_up,
        expert_down,
        shared_gate.T,
        shared_up.T,
        shared_down,
    )


def solution(mesh):
    placed = (
        P("ep", None),
        P(),
        P("ep", None, None),
        P("ep", None, None),
        P("ep", None, None),
        P(None, "ep"),
        P(None, "ep"),
        P("ep", None),
        P(),
        P("ep", None),
        P("ep", None),
    )
    return jax.shard_map(
        per_device, mesh=mesh, in_specs=placed, out_specs=P("ep", None), check_vma=False
    )
```

```python
import functools
import math

import jax
import jax.numpy as jnp
from jax import lax
from jax.experimental import pallas as pl
from jax.experimental.pallas import tpu as pltpu
from jax.sharding import PartitionSpec as P

F32 = jnp.float32
BF16 = jnp.bfloat16


def silu_pair(gate, up):
    return (gate / (1.0 + jnp.exp(-gate)) * up).astype(BF16)


def kernel(
    n,
    plane,
    tokens,
    gain,
    branch,
    route,
    weight,
    e_gate,
    e_up,
    e_down,
    s_gate,
    s_up,
    s_down,
    out,
    toks,
    wg,
    wu,
    wd,
    sgu,
    sd,
    mine,
    theirs,
    given,
    sending,
    landed,
    summed,
    arrived,
    w_sem,
    far_s,
    far_r,
    near_s,
    near_r,
    pass_s,
    pass_r,
    swap_s,
    swap_r,
    part_s,
    part_r,
    last_s,
    last_r,
):
    half = n // 2
    planes = half // plane
    width = tokens.shape[1]
    me = lax.axis_index("ep")
    core = lax.rem(me, 2)
    chip = me // 2
    low = lax.rem(chip, plane)
    high = chip // plane
    partner = {"ep": me + 1 - 2 * core}

    def at(a, b):
        row = lax.rem(high + a + planes, planes)
        column = lax.rem(low + b + plane, plane)
        return {"ep": (row * plane + column) * 2 + core}

    loads = [
        pltpu.make_async_copy(src, dst, w_sem.at[i])
        for i, (src, dst) in enumerate(
            (
                (e_gate.at[0], wg),
                (e_up.at[0], wu),
                (s_gate, sgu.at[0]),
                (s_up, sgu.at[1]),
                (s_down, sd),
                (e_down.at[0], wd),
            )
        )
    ]
    for load in loads:
        load.start()

    barrier = pltpu.get_barrier_semaphore()
    for a in range(1, planes):
        pl.semaphore_signal(barrier, inc=1, device_id=at(a, 0))
    for b in range(1, plane):
        pl.semaphore_signal(barrier, inc=1, device_id=at(0, b))
    pl.semaphore_signal(barrier, inc=1, device_id=partner)

    values = tokens[...].astype(F32)
    scale = lax.rsqrt(jnp.mean(values * values, axis=-1, keepdims=True) + 1e-06)
    normed = (values * scale * gain[...]).astype(BF16)
    score = jnp.sum(
        normed.astype(F32) * branch[...].astype(F32).reshape(1, -1), axis=-1, keepdims=True
    )

    def columns(shape):
        lane = lax.broadcasted_iota(jnp.int32, shape, 1)
        piece = (lane >= n + 1).astype(jnp.int32) + (lane >= 2 * (n + 1)).astype(jnp.int32)
        return piece, lane - piece * (n + 1)

    piece, column = columns((tokens.shape[0], toks.shape[4] - width))
    table = jnp.where(column == n, 1.0 / (1.0 + jnp.exp(-score)), 0.0)
    for k in range(route.shape[1]):
        table += jnp.where(column == route[:, k : k + 1], weight[:, k : k + 1], 0.0)
    first = table.astype(BF16).astype(F32)
    second = (table - first).astype(BF16).astype(F32)
    third = table - first - second
    pieces = jnp.where(piece == 0, first, jnp.where(piece == 1, second, third))
    toks[0, 0, 0, :, :width] = normed
    toks[0, 0, 0, :, width:] = pieces.astype(BF16)

    pl.semaphore_wait(barrier, planes + plane - 1)

    slots = [0] + sorted(range(1, planes), key=lambda a: min(a, planes - a))
    middle = max(1, planes // 2)
    chunks = [c for c in ((0, middle), (middle, planes)) if c[0] < c[1]]
    others = range(1, planes)
    peers = range(1, plane)

    def far(i):
        return pltpu.make_async_remote_copy(
            toks.at[0, 0, 0],
            toks.at[i, 0, 0],
            far_s.at[i],
            far_r.at[i],
            device_id=at(-slots[i], 0),
        )

    def near(i, b):
        return pltpu.make_async_remote_copy(
            toks.at[i, 0, 0],
            toks.at[i, 0, b],
            near_s.at[b, i],
            near_r.at[b, i],
            device_id=at(0, -b),
        )

    def hand(i, b):
        return pltpu.make_async_remote_copy(
            toks.at[i, 0, b],
            toks.at[i, 1, b],
            pass_s.at[b, i],
            pass_r.at[b, i],
            device_id=partner,
        )

    def swap(c):
        low_i, high_i = chunks[c]
        span = pl.ds(low_i, high_i - low_i)
        return pltpu.make_async_remote_copy(
            theirs.at[span], given.at[span], swap_s.at[c], swap_r.at[c], device_id=partner
        )

    def part(i, b):
        return pltpu.make_async_remote_copy(
            sending.at[i, b],
            landed.at[i, b],
            part_s.at[b, i],
            part_r.at[b, i],
            device_id=at(0, b),
        )

    def last(i):
        return pltpu.make_async_remote_copy(
            summed.at[i],
            arrived.at[i],
            last_s.at[i],
            last_r.at[i],
            device_id=at(slots[i], 0),
        )

    def compute(c):
        low_i, high_i = chunks[c]
        count = high_i - low_i
        rows = count * 2 * plane * tokens.shape[0]
        x = toks[low_i:high_i, :, :, :, :width].reshape(rows, width)
        facts = toks[low_i:high_i, :, :, :, width:].astype(F32).reshape(rows, -1)
        _, spot = columns(facts.shape)
        share = jnp.sum(jnp.where(spot == me, facts, 0.0), axis=1, keepdims=True)
        gate = jnp.sum(jnp.where(spot == n, facts, 0.0), axis=1, keepdims=True)
        dot = functools.partial(jnp.dot, preferred_element_type=F32)
        hidden = silu_pair(dot(x, wg[...]), dot(x, wu[...]))
        units = sgu.shape[1]
        pair = lax.dot_general(
            x,
            sgu[...].reshape(2 * units, width),
            (((1,), (1,)), ((), ())),
            preferred_element_type=F32,
        )
        dense_hidden = silu_pair(pair[:, :units], pair[:, units:])
        routed = dot(hidden, wd[...]).astype(BF16).astype(F32)
        both = share * routed + gate * dot(dense_hidden, sd[...])
        both = both.reshape(count, 2, *mine.shape[1:])
        theirs[low_i:high_i] = both[:, 1].astype(BF16)
        mine[low_i:high_i] = both[:, 0]
        swap(c).start()

    def collect(c):
        for i in range(*chunks[c]):
            for b in peers:
                near(i, b).wait_recv()
                hand(i, b).start()

    def ready(c):
        for i in range(*chunks[c]):
            for b in range(plane):
                hand(i, b).wait_recv()

    def depart(c):
        low_i, high_i = chunks[c]
        swap(c).wait_recv()
        mine[low_i:high_i] += given[low_i:high_i].astype(F32)
        for b in peers:
            sending[low_i:high_i, b] = mine[low_i:high_i, b].astype(BF16)
        for i in range(low_i, high_i):
            for b in peers:
                part(i, b).start()

    def whole(i):
        total = mine[i, 0]
        for b in peers:
            part(i, b).wait_recv()
            total += landed[i, b].astype(F32)
        return total

    for i in others:
        far(i).start()
    for b in peers:
        near(0, b).start()
    hand(0, 0).start()
    for i in others:
        far(i).wait_recv()
        for b in peers:
            near(i, b).start()
        hand(i, 0).start()

    collect(0)
    for load in loads:
        load.wait()
    ready(0)
    compute(0)
    for c in range(1, len(chunks)):
        collect(c)
        depart(c - 1)
        ready(c)
        compute(c)
        for i in range(*chunks[c - 1]):
            if i > 0:
                summed[i] = whole(i).astype(BF16)
                last(i).start()
    depart(len(chunks) - 1)
    for i in range(*chunks[-1]):
        if i > 0:
            summed[i] = whole(i).astype(BF16)
            last(i).start()
    result = whole(0)

    for i in range(planes):
        for b in range(plane):
            hand(i, b).wait_send()
            if b > 0:
                near(i, b).wait_send()
                part(i, b).wait_send()
        if i > 0:
            far(i).wait_send()
    for c in range(len(chunks)):
        swap(c).wait_send()

    for i in others:
        last(i).wait_recv()
        result += arrived[i].astype(F32)
    out[...] = result.astype(BF16)
    for i in others:
        last(i).wait_send()


def per_device(
    tokens,
    norm_gain,
    expert_gate,
    expert_up,
    expert_down,
    shared_gate,
    shared_up,
    shared_down,
    branch_gate,
    route_expert,
    route_weight,
):
    n = lax.axis_size("ep")
    half = n // 2
    plane = math.isqrt(half)
    while half % plane:
        plane -= 1
    planes = half // plane
    rows, width = tokens.shape
    lanes = (3 * (n + 1) + 127) // 128 * 128
    vmem = pl.BlockSpec(memory_space=pltpu.VMEM)
    anywhere = pl.BlockSpec(memory_space=pl.ANY)
    dma = pltpu.SemaphoreType.DMA
    blocks = pltpu.VMEM((planes, plane, rows, width), BF16)
    return pl.pallas_call(
        functools.partial(kernel, n, plane),
        out_shape=jax.ShapeDtypeStruct((rows, width), BF16),
        in_specs=[vmem] * 5 + [anywhere] * 6,
        out_specs=vmem,
        scratch_shapes=[
            pltpu.VMEM((planes, 2, plane, rows, width + lanes), BF16),
            pltpu.VMEM(expert_gate.shape[1:], BF16),
            pltpu.VMEM(expert_up.shape[1:], BF16),
            pltpu.VMEM(expert_down.shape[1:], BF16),
            pltpu.VMEM((2,) + shared_gate.shape[::-1], BF16),
            pltpu.VMEM(shared_down.shape, BF16),
            pltpu.VMEM((planes, plane, rows, width), F32),
            blocks,
            blocks,
            blocks,
            blocks,
            pltpu.VMEM((planes, rows, width), BF16),
            pltpu.VMEM((planes, rows, width), BF16),
            dma((6,)),
            dma((planes,)),
            dma((planes,)),
            dma((plane, planes)),
            dma((plane, planes)),
            dma((plane, planes)),
            dma((plane, planes)),
            dma((2,)),
            dma((2,)),
            dma((plane, planes)),
            dma((plane, planes)),
            dma((planes,)),
            dma((planes,)),
        ],
        compiler_params=pltpu.CompilerParams(
            collective_id=0, has_side_effects=True, vmem_limit_bytes=60 * 1024 * 1024
        ),
    )(
        tokens,
        norm_gain.reshape(1, -1),
        branch_gate,
        route_expert,
        route_weight,
        expert_gate,
        expert_up,
        expert_down,
        shared_gate.T,
        shared_up.T,
        shared_down,
    )


def solution(mesh):
    placed = (
        P("ep", None),
        P(),
        P("ep", None, None),
        P("ep", None, None),
        P("ep", None, None),
        P(None, "ep"),
        P(None, "ep"),
        P("ep", None),
        P(),
        P("ep", None),
        P("ep", None),
    )
    return jax.shard_map(
        per_device, mesh=mesh, in_specs=placed, out_specs=P("ep", None), check_vma=False
    )
```

```python
import functools
import math

import jax
import jax.numpy as jnp
from jax import lax
from jax.experimental import pallas as pl
from jax.experimental.pallas import tpu as pltpu
from jax.sharding import PartitionSpec as P

F32 = jnp.float32
BF16 = jnp.bfloat16


def silu_pair(gate, up):
    return (gate / (1.0 + jnp.exp(-gate)) * up).astype(BF16)


def kernel(
    n,
    plane,
    tokens,
    gain,
    branch,
    route,
    weight,
    e_gate,
    e_up,
    e_down,
    s_gate,
    s_up,
    s_down,
    out,
    toks,
    wg,
    wu,
    wd,
    sgu,
    sd,
    mine,
    theirs,
    given,
    sending,
    landed,
    summed,
    arrived,
    w_sem,
    far_s,
    far_r,
    near_s,
    near_r,
    pass_s,
    pass_r,
    swap_s,
    swap_r,
    part_s,
    part_r,
    last_s,
    last_r,
):
    half = n // 2
    planes = half // plane
    width = tokens.shape[1]
    me = lax.axis_index("ep")
    core = lax.rem(me, 2)
    chip = me // 2
    low = lax.rem(chip, plane)
    high = chip // plane
    partner = {"ep": me + 1 - 2 * core}

    def at(a, b):
        row = lax.rem(high + a + planes, planes)
        column = lax.rem(low + b + plane, plane)
        return {"ep": (row * plane + column) * 2 + core}

    loads = [
        pltpu.make_async_copy(src, dst, w_sem.at[i])
        for i, (src, dst) in enumerate(
            (
                (e_gate.at[0], wg),
                (e_up.at[0], wu),
                (s_gate, sgu.at[0]),
                (s_up, sgu.at[1]),
                (s_down, sd),
                (e_down.at[0], wd),
            )
        )
    ]
    for load in loads:
        load.start()

    barrier = pltpu.get_barrier_semaphore()
    for a in range(1, planes):
        pl.semaphore_signal(barrier, inc=1, device_id=at(a, 0))
    for b in range(1, plane):
        pl.semaphore_signal(barrier, inc=1, device_id=at(0, b))
    pl.semaphore_signal(barrier, inc=1, device_id=partner)

    values = tokens[...].astype(F32)
    scale = lax.rsqrt(jnp.mean(values * values, axis=-1, keepdims=True) + 1e-06)
    normed = (values * scale * gain[...]).astype(BF16)
    score = jnp.sum(
        normed.astype(F32) * branch[...].astype(F32).reshape(1, -1), axis=-1, keepdims=True
    )

    def columns(shape):
        lane = lax.broadcasted_iota(jnp.int32, shape, 1)
        piece = (lane >= n + 1).astype(jnp.int32) + (lane >= 2 * (n + 1)).astype(jnp.int32)
        return piece, lane - piece * (n + 1)

    piece, column = columns((tokens.shape[0], toks.shape[4] - width))
    table = jnp.where(column == n, 1.0 / (1.0 + jnp.exp(-score)), 0.0)
    for k in range(route.shape[1]):
        table += jnp.where(column == route[:, k : k + 1], weight[:, k : k + 1], 0.0)
    first = table.astype(BF16).astype(F32)
    second = (table - first).astype(BF16).astype(F32)
    third = table - first - second
    pieces = jnp.where(piece == 0, first, jnp.where(piece == 1, second, third))
    toks[0, 0, 0, :, :width] = normed
    toks[0, 0, 0, :, width:] = pieces.astype(BF16)

    pl.semaphore_wait(barrier, planes + plane - 1)

    slots = [0] + sorted(range(1, planes), key=lambda a: min(a, planes - a))
    middle = max(1, planes // 2)
    chunks = [c for c in ((0, middle), (middle, planes)) if c[0] < c[1]]
    others = range(1, planes)
    peers = range(1, plane)

    def far(i):
        return pltpu.make_async_remote_copy(
            toks.at[0, 0, 0],
            toks.at[i, 0, 0],
            far_s.at[i],
            far_r.at[i],
            device_id=at(-slots[i], 0),
        )

    def near(i, b):
        return pltpu.make_async_remote_copy(
            toks.at[i, 0, 0],
            toks.at[i, 0, b],
            near_s.at[b, i],
            near_r.at[b, i],
            device_id=at(0, -b),
        )

    def hand(i, b):
        return pltpu.make_async_remote_copy(
            toks.at[i, 0, b],
            toks.at[i, 1, b],
            pass_s.at[b, i],
            pass_r.at[b, i],
            device_id=partner,
        )

    def swap(c):
        low_i, high_i = chunks[c]
        span = pl.ds(low_i, high_i - low_i)
        return pltpu.make_async_remote_copy(
            theirs.at[span], given.at[span], swap_s.at[c], swap_r.at[c], device_id=partner
        )

    def part(i, b):
        return pltpu.make_async_remote_copy(
            sending.at[i, b],
            landed.at[i, b],
            part_s.at[b, i],
            part_r.at[b, i],
            device_id=at(0, b),
        )

    def last(i):
        return pltpu.make_async_remote_copy(
            summed.at[i],
            arrived.at[i],
            last_s.at[i],
            last_r.at[i],
            device_id=at(slots[i], 0),
        )

    def compute(c):
        low_i, high_i = chunks[c]
        count = high_i - low_i
        rows = count * 2 * plane * tokens.shape[0]
        x = toks[low_i:high_i, :, :, :, :width].reshape(rows, width)
        facts = toks[low_i:high_i, :, :, :, width:].astype(F32).reshape(rows, -1)
        _, spot = columns(facts.shape)
        share = jnp.sum(jnp.where(spot == me, facts, 0.0), axis=1, keepdims=True)
        gate = jnp.sum(jnp.where(spot == n, facts, 0.0), axis=1, keepdims=True)
        dot = functools.partial(jnp.dot, preferred_element_type=F32)
        hidden = silu_pair(dot(x, wg[...]), dot(x, wu[...]))
        units = sgu.shape[1]
        pair = lax.dot_general(
            x,
            sgu[...].reshape(2 * units, width),
            (((1,), (1,)), ((), ())),
            preferred_element_type=F32,
        )
        dense_hidden = silu_pair(pair[:, :units], pair[:, units:])
        routed = dot(hidden, wd[...]).astype(BF16).astype(F32)
        both = share * routed + gate * dot(dense_hidden, sd[...])
        both = both.reshape(count, 2, *mine.shape[1:])
        theirs[low_i:high_i] = both[:, 1].astype(BF16)
        mine[low_i:high_i] = both[:, 0]
        swap(c).start()

    def collect(c):
        for i in range(*chunks[c]):
            for b in peers:
                near(i, b).wait_recv()
                hand(i, b).start()

    def ready(c):
        for i in range(*chunks[c]):
            for b in range(plane):
                hand(i, b).wait_recv()

    def depart(c):
        low_i, high_i = chunks[c]
        swap(c).wait_recv()
        for i in range(high_i - 1, low_i - 1, -1):
            for b in peers:
                sending[i, b] = (mine[i, b] + given[i, b].astype(F32)).astype(BF16)
        for i in range(high_i - 1, low_i - 1, -1):
            for b in peers:
                part(i, b).start()

    def whole(i):
        total = mine[i, 0] + given[i, 0].astype(F32)
        for b in peers:
            part(i, b).wait_recv()
            total += landed[i, b].astype(F32)
        return total

    for i in others:
        far(i).start()
    for b in peers:
        near(0, b).start()
    hand(0, 0).start()
    for i in others:
        far(i).wait_recv()
        for b in peers:
            near(i, b).start()
        hand(i, 0).start()

    collect(0)
    for load in loads:
        load.wait()
    ready(0)
    compute(0)
    for c in range(1, len(chunks)):
        collect(c)
        depart(c - 1)
        ready(c)
        compute(c)
        for i in reversed(range(*chunks[c - 1])):
            if i > 0:
                summed[i] = whole(i).astype(BF16)
                last(i).start()
    depart(len(chunks) - 1)
    for i in reversed(range(*chunks[-1])):
        if i > 0:
            summed[i] = whole(i).astype(BF16)
            last(i).start()
    result = whole(0)

    for i in range(planes):
        for b in range(plane):
            hand(i, b).wait_send()
            if b > 0:
                near(i, b).wait_send()
                part(i, b).wait_send()
        if i > 0:
            far(i).wait_send()
    for c in range(len(chunks)):
        swap(c).wait_send()

    for i in others:
        last(i).wait_recv()
        result += arrived[i].astype(F32)
    out[...] = result.astype(BF16)
    for i in others:
        last(i).wait_send()


def per_device(
    tokens,
    norm_gain,
    expert_gate,
    expert_up,
    expert_down,
    shared_gate,
    shared_up,
    shared_down,
    branch_gate,
    route_expert,
    route_weight,
):
    n = lax.axis_size("ep")
    half = n // 2
    plane = math.isqrt(half)
    while half % plane:
        plane -= 1
    planes = half // plane
    rows, width = tokens.shape
    lanes = (3 * (n + 1) + 127) // 128 * 128
    vmem = pl.BlockSpec(memory_space=pltpu.VMEM)
    anywhere = pl.BlockSpec(memory_space=pl.ANY)
    dma = pltpu.SemaphoreType.DMA
    blocks = pltpu.VMEM((planes, plane, rows, width), BF16)
    return pl.pallas_call(
        functools.partial(kernel, n, plane),
        out_shape=jax.ShapeDtypeStruct((rows, width), BF16),
        in_specs=[vmem] * 5 + [anywhere] * 6,
        out_specs=vmem,
        scratch_shapes=[
            pltpu.VMEM((planes, 2, plane, rows, width + lanes), BF16),
            pltpu.VMEM(expert_gate.shape[1:], BF16),
            pltpu.VMEM(expert_up.shape[1:], BF16),
            pltpu.VMEM(expert_down.shape[1:], BF16),
            pltpu.VMEM((2,) + shared_gate.shape[::-1], BF16),
            pltpu.VMEM(shared_down.shape, BF16),
            pltpu.VMEM((planes, plane, rows, width), F32),
            blocks,
            blocks,
            blocks,
            blocks,
            pltpu.VMEM((planes, rows, width), BF16),
            pltpu.VMEM((planes, rows, width), BF16),
            dma((6,)),
            dma((planes,)),
            dma((planes,)),
            dma((plane, planes)),
            dma((plane, planes)),
            dma((plane, planes)),
            dma((plane, planes)),
            dma((2,)),
            dma((2,)),
            dma((plane, planes)),
            dma((plane, planes)),
            dma((planes,)),
            dma((planes,)),
        ],
        compiler_params=pltpu.CompilerParams(
            collective_id=0, has_side_effects=True, vmem_limit_bytes=60 * 1024 * 1024
        ),
    )(
        tokens,
        norm_gain.reshape(1, -1),
        branch_gate,
        route_expert,
        route_weight,
        expert_gate,
        expert_up,
        expert_down,
        shared_gate.T,
        shared_up.T,
        shared_down,
    )


def solution(mesh):
    placed = (
        P("ep", None),
        P(),
        P("ep", None, None),
        P("ep", None, None),
        P("ep", None, None),
        P(None, "ep"),
        P(None, "ep"),
        P("ep", None),
        P(),
        P("ep", None),
        P("ep", None),
    )
    return jax.shard_map(
        per_device, mesh=mesh, in_specs=placed, out_specs=P("ep", None), check_vma=False
    )
```
